32 devices in a mesh: sp: 8 (over z, x), tp: 4 (over y, core).
Axes of the slice: x: 2, y: 2, z: 4, core: 2. Of those that a mesh axis runs over, the one named last changes fastest.
Arguments:
- tokens: bfloat16 [2048, 4096], P('sp', 'tp'), may hold values from -6 to 6
- pre_gain: float32 [4096], replicated, may hold values from 0.1 to 1.9
- rate_factor: float32 [2048], P('sp'), may hold values from 0.5 to 2, as said below
- w_rec_in: bfloat16 [4096, 1024], P(None, 'tp'), may hold values from -0.09375 to 0.09375
- w_rec_gate: bfloat16 [4096, 1024], P(None, 'tp')
- conv_taps: float32 [4, 1024], P(None, 'tp'), may hold values from -3 to 3
- rate_maps: bfloat16 [8, 128, 128], P('tp'), may hold values from -0.5 to 0.5
- input_maps: bfloat16 [8, 128, 128], P('tp'), may hold values from -0.5 to 0.5
- decay_param: float32 [1024], P('tp'), as said below
- w_query: bfloat16 [4096, 1536], P(None, 'tp'), may hold values from -0.09375 to 0.09375
- w_latent: bfloat16 [4096, 512], replicated, may hold values from -0.09375 to 0.09375
- w_rope_key: bfloat16 [4096, 64], replicated, may hold values from -0.09375 to 0.09375
- latent_gain: float32 [512], replicated, may hold values from 0.7 to 100, as said below
- w_expand: bfloat16 [512, 2048], P(None, 'tp')
- rec_gain: float32 [1024], P('tp'), may hold values from 0.1 to 1.9
- att_gain: float32 [1024], P('tp'), may hold values from 0.1 to 1.9
- w_out_rec: bfloat16 [1024, 4096], P('tp'), may hold values from -0.125 to 0.125
- w_out_att: bfloat16 [1024, 4096], P('tp'), may hold values from -0.125 to 0.125
- post_gain: float32 [4096], replicated, may hold values from 0.1 to 1.9
Outputs:
- layer_out: bfloat16 [2048, 4096], P(('sp', 'tp'))
The draws below stay inside these ranges and needn't reach their ends.
Inputs may be any that keep to these rules, and one draw needn't show every extreme that they name: `rate_factor`: one positive factor for each position. `decay_param`: one parameter for each recurrent channel. `latent_gain`: one positive gain for each latent entry.
All inputs are finite; a program needn't handle non-finite values.
Results may differ from the reference program's by a relative error of at most 0.017.
The reference program's roundings to bfloat16 on the way count: a program that leaves them out, or rounds other values in their place, can miss the bound.
Values may be sent and summed in bfloat16 or wider, within the bound.
A program may use at most 128 MiB of HBM per device.

```python
import math
import jax
import jax.numpy as jnp
from jax import lax

D = 4096
LRU_W = 1024
LRU_BLK = 128
CONV = 4
HEADS = 8
NOPE = 128
ROPE = 64
VDIM = 128
LATENT = 512
TOK_DEV = 256
SEQ = 2048
N_TP = 4


def draw_rate_factor(key, part):
    span_rows = max(TOK_DEV // 2, 1)
    levels = jnp.exp(jax.random.uniform(key, (SEQ // span_rows,), jnp.float32, math.log(0.5), math.log(2.0)))
    return jnp.repeat(levels, span_rows, total_repeat_length=SEQ)


def draw_decay_param(key, part):
    choose_key, slow_key, fast_key = jax.random.split(key, 3)
    share = 0.5
    slow_mask = jax.random.uniform(choose_key, (LRU_W,), jnp.float32) < share
    slow_value = math.log(8.0 * SEQ) + jax.random.uniform(slow_key, (LRU_W,), jnp.float32, 0.5, 2.0)
    fast_value = jax.random.uniform(fast_key, (LRU_W,), jnp.float32, 4.5, 6.0)
    return jnp.where(slow_mask, slow_value, fast_value)


def draw_latent_gain(key, part):
    return jax.random.uniform(key, (LATENT,), jnp.float32, 0.7, 1.3)


def draw_w_rec_gate(key, part):
    base_key, factor_key = jax.random.split(key)
    base = jax.random.normal(base_key, (D, LRU_W), jnp.float32) / math.sqrt(D)
    factors = jnp.exp(jax.random.uniform(factor_key, (LRU_W // LRU_BLK,), jnp.float32, math.log(1.0 / 3.0), math.log(3.0)))
    return (base * jnp.repeat(factors, LRU_BLK, total_repeat_length=LRU_W)[None, :]).astype(jnp.bfloat16)


def draw_w_expand(key, part):
    base_key, factor_key = jax.random.split(key)
    base = jax.random.normal(base_key, (LATENT, HEADS, NOPE + VDIM), jnp.float32) / math.sqrt(LATENT)
    factors = jnp.exp(jax.random.uniform(factor_key, (HEADS,), jnp.float32, math.log(1.0 / 3.0), math.log(3.0)))
    columns = jnp.arange(NOPE + VDIM)
    scaling = jnp.where(columns[None, :] >= NOPE, factors[:, None], 1.0)
    return (base * scaling[None, :, :]).reshape(LATENT, HEADS * (NOPE + VDIM)).astype(jnp.bfloat16)


def level_of(own_key, dims, cuts, low, high):
    level = 1.0
    for dim, shards_of in cuts:
        steps = jax.random.uniform(jax.random.fold_in(jax.random.fold_in(own_key, 6), dim), (shards_of,), jnp.float32, low / len(cuts), high / len(cuts))
        level = level * jnp.repeat(jnp.exp(steps), dims[dim] // shards_of).reshape((-1,) + (1,) * (len(dims) - 1 - dim))
    return level


def scatter_about(stream_key, shape, width, reach, shards=(), held_as=jnp.bfloat16):
    drawn = jax.random.normal(stream_key, shape, jnp.float32) * width
    if len(shards) > 0:
        drawn = level_of(stream_key, shape, shards, -0.22, 0.18) * drawn
    return jnp.clip(drawn, min=-reach, max=reach).astype(held_as)


def setup_inputs(seed: int = 0) -> dict:
    key_list = jax.random.split(jax.random.key(seed), 20)
    tokens = scatter_about(key_list[0], (SEQ, D), 1.0, 6.0, ((0, 8), (1, 4)))
    pre_gain = jnp.clip(1.0 + 0.18 * jax.random.normal(key_list[1], (D,), jnp.float32), 0.1, 1.9)
    rate_factor = draw_rate_factor(jax.random.fold_in(key_list[19], 71), 0)
    w_rec_in = scatter_about(key_list[3], (D, LRU_W), D ** -0.5, 0.09375, ((1, 4),))
    w_rec_gate = draw_w_rec_gate(jax.random.fold_in(key_list[19], 71), 0)
    conv_taps = scatter_about(key_list[5], (CONV, LRU_W), 0.5, 3.0, ((1, 4),), jnp.float32)
    rate_maps = scatter_about(key_list[6], (LRU_W // LRU_BLK, LRU_BLK, LRU_BLK), LRU_BLK ** -0.5, 0.5, ((0, 4),))
    input_maps = scatter_about(key_list[7], (LRU_W // LRU_BLK, LRU_BLK, LRU_BLK), LRU_BLK ** -0.5, 0.5, ((0, 4),))
    decay_param = draw_decay_param(jax.random.fold_in(key_list[19], 71), 0)
    w_query = scatter_about(key_list[9], (D, HEADS * (NOPE + ROPE)), D ** -0.5, 0.09375, ((1, 4),))
    w_latent = scatter_about(key_list[10], (D, LATENT), D ** -0.5, 0.09375)
    w_rope_key = scatter_about(key_list[11], (D, ROPE), D ** -0.5, 0.09375)
    latent_gain = draw_latent_gain(jax.random.fold_in(key_list[19], 71), 0)
    w_expand = draw_w_expand(jax.random.fold_in(key_list[19], 71), 0)
    rec_gain = jnp.clip(1.0 + 0.18 * jax.random.normal(key_list[14], (LRU_W,), jnp.float32), 0.1, 1.9)
    att_gain = jnp.clip(1.0 + 0.18 * jax.random.normal(key_list[15], (HEADS * VDIM,), jnp.float32), 0.1, 1.9)
    w_out_rec = scatter_about(key_list[16], (LRU_W, D), (LRU_W + HEADS * VDIM) ** -0.5, 0.125, ((0, 4),))
    w_out_att = scatter_about(key_list[17], (HEADS * VDIM, D), (LRU_W + HEADS * VDIM) ** -0.5, 0.125, ((0, 4),))
    post_gain = jnp.clip(1.0 + 0.18 * jax.random.normal(key_list[18], (D,), jnp.float32), 0.1, 1.9)
    return {"tokens": tokens, "pre_gain": pre_gain, "rate_factor": rate_factor, "w_rec_in": w_rec_in, "w_rec_gate": w_rec_gate, "conv_taps": conv_taps, "rate_maps": rate_maps, "input_maps": input_maps, "decay_param": decay_param, "w_query": w_query, "w_latent": w_latent, "w_rope_key": w_rope_key, "latent_gain": latent_gain, "w_expand": w_expand, "rec_gain": rec_gain, "att_gain": att_gain, "w_out_rec": w_out_rec, "w_out_att": w_out_att, "post_gain": post_gain}


EPS = 1e-06
RATE_C = 8.0
THETA = 10000.0

def rms_inverse(values):
    return lax.rsqrt(lax.optimization_barrier(jnp.mean(values * values, axis=-1, keepdims=True)) + EPS)

def rotate(values, cosine, sine_part):
    half_width = values.shape[-1] // 2
    leading = values[..., :half_width]
    trailing = values[..., half_width:]
    return jnp.concatenate([leading * cosine - trailing * sine_part, trailing * cosine + leading * sine_part], axis=-1)

def angles(length, offset, span_width):
    frequency = 1.0 / THETA ** (jnp.arange(0, span_width, 2).astype(jnp.float32) / span_width)
    places = (offset + jnp.arange(length).astype(jnp.int32)).astype(jnp.float32)
    turned = places[:, None] * frequency[None, :]
    return (jnp.cos(turned), jnp.sin(turned))

def combine_steps(earlier, later):
    return (earlier[0] * later[0], later[0] * earlier[1] + later[1])

def attend_block(state_now, query_nope, query_rope, places, keys_nope, key_rope, values, key_root):
    maxima, totals, accumulated = state_now
    scaling = 1.0 / math.sqrt(query_nope.shape[-1] + query_rope.shape[-1])
    scores = jnp.einsum('qhd,khd->hqk', query_nope.astype(jnp.float32), keys_nope.astype(jnp.float32))
    scores = scores + jnp.einsum('qhd,kd->hqk', query_rope.astype(jnp.float32), key_rope.astype(jnp.float32))
    scores = scores * scaling
    key_places = key_root + jnp.arange(keys_nope.shape[0]).astype(jnp.int32)
    visible = key_places[None, :] <= places[:, None]
    scores = jnp.where(visible[None], scores, -jnp.inf)
    largest = jnp.maximum(maxima, lax.optimization_barrier(jnp.max(scores, axis=-1)))
    anchor = jnp.where(largest == -jnp.inf, 0.0, largest)
    weights = jnp.exp(scores - anchor[..., None])
    shrink = jnp.exp(maxima - anchor)
    totals = totals * shrink + lax.optimization_barrier(jnp.sum(weights, axis=-1))
    rounded = weights.astype(jnp.bfloat16).astype(jnp.float32)
    accumulated = accumulated * shrink[..., None] + jnp.einsum('hqk,khd->hqd', rounded, values.astype(jnp.float32))
    return (largest, totals, accumulated)

def reference(tokens, pre_gain, rate_factor, w_rec_in, w_rec_gate, conv_taps, rate_maps, input_maps, decay_param, w_query, w_latent, w_rope_key, latent_gain, w_expand, rec_gain, att_gain, w_out_rec, w_out_att, post_gain):
    tokens_wide = tokens.astype(jnp.float32)
    inverse = rms_inverse(tokens_wide)
    scaled = (tokens_wide * pre_gain).astype(jnp.bfloat16)

    def project(weight):
        return inverse * jnp.dot(scaled, weight, preferred_element_type=jnp.float32)
    rec_input = project(w_rec_in).astype(jnp.bfloat16)
    gate_value = project(w_rec_gate)
    query_raw = project(w_query)
    latent_raw = project(w_latent)
    rope_raw = project(w_rope_key)
    padded = jnp.concatenate([jnp.zeros((CONV - 1, LRU_W), jnp.bfloat16), rec_input], axis=0)
    convolved = conv_taps[0] * padded[0:SEQ].astype(jnp.float32)
    for tap_index in range(1, CONV):
        convolved = convolved + conv_taps[tap_index] * padded[tap_index:tap_index + SEQ].astype(jnp.float32)
    conv_low = lax.optimization_barrier(convolved.astype(jnp.bfloat16)).astype(jnp.float32)
    blocks = conv_low.reshape(SEQ, LRU_W // LRU_BLK, LRU_BLK)
    rate_gate = jax.nn.sigmoid(jnp.einsum('sbi,bij->sbj', blocks, rate_maps.astype(jnp.float32))).reshape(SEQ, LRU_W)
    entry_gate = jax.nn.sigmoid(jnp.einsum('sbi,bij->sbj', blocks, input_maps.astype(jnp.float32))).reshape(SEQ, LRU_W)
    log_keep = -RATE_C * rate_factor[:, None] * rate_gate * jax.nn.softplus(-decay_param)
    keep_rate = jnp.exp(log_keep)
    driven = jnp.sqrt(-jnp.expm1(2.0 * log_keep)) * entry_gate * convolved
    state_seq = lax.associative_scan(combine_steps, (keep_rate, driven), axis=0)[1]
    rec_out = state_seq * jax.nn.gelu(gate_value)
    rec_norm = (rec_out * rms_inverse(rec_out) * rec_gain).astype(jnp.bfloat16)
    cosine, sine_part = angles(SEQ, 0, ROPE)
    query_heads = query_raw.reshape(SEQ, HEADS, NOPE + ROPE)
    query_nope = query_heads[:, :, :NOPE].astype(jnp.bfloat16)
    query_rope = rotate(query_heads[:, :, NOPE:], cosine[:, None, :], sine_part[:, None, :]).astype(jnp.bfloat16)
    latent_norm = (latent_raw * rms_inverse(latent_raw) * latent_gain).astype(jnp.bfloat16)
    rope_key = rotate(rope_raw, cosine, sine_part).astype(jnp.bfloat16)
    expanded = jnp.dot(latent_norm, w_expand, preferred_element_type=jnp.float32).astype(jnp.bfloat16)
    expanded = expanded.reshape(SEQ, HEADS, NOPE + VDIM)
    keys_nope = expanded[:, :, :NOPE]
    values = expanded[:, :, NOPE:]
    query_span = math.gcd(SEQ, 256)
    block_count = SEQ // query_span

    def one_block(block_index):
        root = block_index * query_span
        block_nope = lax.dynamic_slice_in_dim(query_nope, root, query_span, 0)
        block_rope = lax.dynamic_slice_in_dim(query_rope, root, query_span, 0)
        places = root + jnp.arange(query_span).astype(jnp.int32)
        initial = (jnp.full((HEADS, query_span), -jnp.inf, jnp.float32), jnp.zeros((HEADS, query_span), jnp.float32), jnp.zeros((HEADS, query_span, VDIM), jnp.float32))
        maxima, totals, accumulated = attend_block(initial, block_nope, block_rope, places, keys_nope, rope_key, values, 0)
        return (accumulated / totals[..., None]).transpose(1, 0, 2)
    att_out = lax.map(one_block, jnp.arange(block_count).astype(jnp.int32)).reshape(SEQ, HEADS * VDIM)
    att_norm = (att_out * rms_inverse(att_out) * att_gain).astype(jnp.bfloat16)
    rec_width = LRU_W // N_TP
    att_width = HEADS * VDIM // N_TP
    mixed_sum = jnp.zeros((SEQ, D), jnp.float32)
    for member in range(N_TP):
        partial_value = jnp.dot(rec_norm[:, member * rec_width:(member + 1) * rec_width], w_out_rec[member * rec_width:(member + 1) * rec_width], preferred_element_type=jnp.float32)
        partial_value = partial_value + jnp.dot(att_norm[:, member * att_width:(member + 1) * att_width], w_out_att[member * att_width:(member + 1) * att_width], preferred_element_type=jnp.float32)
        mixed_sum = mixed_sum + lax.optimization_barrier(partial_value.astype(jnp.bfloat16)).astype(jnp.float32)
    return (mixed_sum * rms_inverse(mixed_sum) * post_gain).astype(jnp.bfloat16)
```

```python
import functools
import math

import jax
import jax.numpy as jnp
from jax import lax
from jax.experimental import pallas as pl
from jax.experimental.pallas import tpu as pltpu
from jax.sharding import PartitionSpec as P

NOPE = 128
ROPE = 64
VDIM = 128


EPS = 1e-06
RATE_C = 8.0
THETA = 10000.0
span_limit = 2048


def passed_along(block, axis, distance):
    devices = range(lax.axis_size(axis))
    route = [(i - distance, i) for i in devices if i - distance in devices]
    return lax.ppermute(block, axis, route)


def entering(value, axis, join, neutral):
    count, mine = (lax.axis_size(axis), lax.axis_index(axis))
    pieces = jax.tree.map(lambda part: lax.all_gather(part, axis), value)
    subtotal = jax.tree.map(
        lambda part, zero: jnp.full_like(part, 0) + jnp.asarray(zero, part.dtype), value, neutral
    )

    def step(position, subtotal):
        longer = join(subtotal, jax.tree.map(lambda part: part[position], pieces))
        return jax.tree.map(lambda new, old: jnp.where(position < mine, new, old), longer, subtotal)

    return lax.fori_loop(0, count - 1, step, subtotal)


def rms_inverse(values):
    return lax.rsqrt(jnp.mean(values * values, axis=-1, keepdims=True) + EPS)


def rotate(values, cosine, sine_part):
    half_width = values.shape[-1] // 2
    leading = values[..., :half_width]
    trailing = values[..., half_width:]
    return jnp.concatenate(
        [leading * cosine - trailing * sine_part, trailing * cosine + leading * sine_part], axis=-1
    )


def angles(length, offset, span_width):
    frequency = 1.0 / THETA ** (jnp.arange(0, span_width, 2).astype(jnp.float32) / span_width)
    places = (offset + jnp.arange(length)).astype(jnp.float32)
    turned = places[:, None] * frequency[None, :]
    return (jnp.cos(turned), jnp.sin(turned))


def combine_steps(earlier, later):
    return (earlier[0] * later[0], later[0] * earlier[1] + later[1])


def attend_block(state_now, query_nope, query_rope, places, keys_nope, key_rope, values, key_root):
    maxima, totals, accumulated = state_now
    scaling = 1.0 / math.sqrt(query_nope.shape[-1] + query_rope.shape[-1])
    scores = jnp.einsum("qhd,khd->hqk", query_nope, keys_nope, preferred_element_type=jnp.float32)
    scores = scores + jnp.einsum(
        "qhd,kd->hqk", query_rope, key_rope, preferred_element_type=jnp.float32
    )
    scores = scores * scaling
    key_places = key_root + jnp.arange(keys_nope.shape[0])
    visible = key_places[None, :] <= places[:, None]
    scores = jnp.where(visible[None], scores, -jnp.inf)
    largest = jnp.maximum(maxima, jnp.max(scores, axis=-1))
    anchor = jnp.where(largest == -jnp.inf, 0.0, largest)
    weights = jnp.exp(scores - anchor[..., None])
    shrink = jnp.exp(maxima - anchor)
    totals = totals * shrink + jnp.sum(weights, axis=-1)
    accumulated = accumulated * shrink[..., None] + jnp.einsum(
        "hqk,khd->hqd", weights.astype(jnp.bfloat16), values, preferred_element_type=jnp.float32
    )
    return (largest, totals, accumulated)


MESH = pl.DeviceIdType.MESH


def one_minus_exp(y):
    series = 1.0 + y * (1.0 / 8.0)
    for order in (7, 6, 5, 4, 3, 2):
        series = 1.0 + y * (1.0 / order) * series
    return jnp.where(y > -0.5, -y * series, 1.0 - jnp.exp(y))


def gelu_tanh(x):
    inner = math.sqrt(2.0 / math.pi) * (x + 0.044715 * (x * x * x))
    return 0.5 * x * (1.0 + jnp.tanh(inner))


def rec_kernel(
    n, rec_ref, taps_ref, rmap_ref, imap_ref, soft_ref, rate_ref, gate_ref,
    out_ref, sq_ref, padded, tail_tx, tail_rx, carry_tx, carry_rx, sems, rsems,
):
    me = lax.axis_index("sp")
    rows, channels = rec_ref.shape
    barrier = pltpu.get_barrier_semaphore()
    for d in range(1, n):
        pl.semaphore_signal(
            barrier, inc=1, device_id={"sp": lax.rem(me + d, n)}, device_id_type=MESH
        )
    x = rec_ref[...].astype(jnp.float32)
    tail_tx[...] = x[rows - 8 :, :]
    padded[8:, :] = x
    pl.semaphore_wait(barrier, n - 1)
    tail = pltpu.make_async_remote_copy(
        src_ref=tail_tx, dst_ref=tail_rx, send_sem=sems.at[0], recv_sem=rsems.at[0],
        device_id={"sp": lax.rem(me + 1, n)}, device_id_type=MESH,
    )
    tail.start()
    tail.wait()
    padded[0:8, :] = jnp.where(me > 0, tail_rx[...], 0.0)
    count = taps_ref.shape[0]
    conv = taps_ref[0:1, :] * padded[9 - count : 9 - count + rows, :]
    for k in range(1, count):
        conv = conv + taps_ref[k : k + 1, :] * padded[9 - count + k : 9 - count + k + rows, :]
    low = conv.astype(jnp.bfloat16)
    width = rmap_ref.shape[1]
    rate, entry = [], []
    for b in range(rmap_ref.shape[0]):
        part = low[:, b * width : (b + 1) * width]
        rate.append(jnp.dot(part, rmap_ref[b], preferred_element_type=jnp.float32))
        entry.append(jnp.dot(part, imap_ref[b], preferred_element_type=jnp.float32))
    rate = jax.nn.sigmoid(jnp.concatenate(rate, axis=1))
    entry = jax.nn.sigmoid(jnp.concatenate(entry, axis=1))
    log_keep = -RATE_C * rate_ref[...] * rate * soft_ref[...]
    a = jnp.exp(log_keep)
    b = jnp.sqrt(one_minus_exp(2.0 * log_keep)) * entry * conv
    row = lax.broadcasted_iota(jnp.int32, (rows, channels), 0)
    d = 1
    while d < rows:
        inside = row >= d
        b = a * jnp.where(inside, pltpu.roll(b, d, 0), 0.0) + b
        a = a * jnp.where(inside, pltpu.roll(a, d, 0), 1.0)
        d *= 2
    carry_tx[...] = jnp.zeros_like(carry_tx)
    carry_tx[0:1, :] = a[rows - 1 :, :]
    carry_tx[1:2, :] = b[rows - 1 :, :]
    copies = []
    for d in range(1, n):
        copies.append(
            pltpu.make_async_remote_copy(
                src_ref=carry_tx, dst_ref=carry_rx.at[me], send_sem=sems.at[d],
                recv_sem=rsems.at[d], device_id={"sp": lax.rem(me + d, n)}, device_id_type=MESH,
            )
        )
        copies[-1].start()
    gated = gelu_tanh(gate_ref[...])
    for copy in copies:
        copy.wait()
    carried = jnp.zeros((1, channels), jnp.float32)
    for s in range(n - 1):
        longer = carry_rx[s, 0:1, :] * carried + carry_rx[s, 1:2, :]
        carried = jnp.where(s < me, longer, carried)
    rec_out = (b + a * carried) * gated
    out_ref[...] = rec_out
    sq_ref[...] = jnp.sum(rec_out * rec_out, axis=1, keepdims=True)


def recurrent(rec_input, conv_taps, rate_maps, input_maps, soft, rate, gate_value):
    n = lax.axis_size("sp")
    rows, channels = rec_input.shape
    vmem = pl.BlockSpec(memory_space=pltpu.VMEM)
    return pl.pallas_call(
        functools.partial(rec_kernel, n),
        out_shape=(
            jax.ShapeDtypeStruct((rows, channels), jnp.float32),
            jax.ShapeDtypeStruct((rows, 1), jnp.float32),
        ),
        in_specs=[vmem] * 7,
        out_specs=(vmem, vmem),
        scratch_shapes=[
            pltpu.VMEM((rows + 8, channels), jnp.float32),
            pltpu.VMEM((8, channels), jnp.float32),
            pltpu.VMEM((8, channels), jnp.float32),
            pltpu.VMEM((8, channels), jnp.float32),
            pltpu.VMEM((n, 8, channels), jnp.float32),
            pltpu.SemaphoreType.DMA((n,)),
            pltpu.SemaphoreType.DMA((n,)),
        ],
        compiler_params=pltpu.CompilerParams(collective_id=0, has_side_effects=True),
        cost_estimate=pl.CostEstimate(flops=20_000_000, bytes_accessed=2_000_000, transcendentals=0),
        name="recurrent",
    )(rec_input, conv_taps, rate_maps, input_maps, soft, rate, gate_value)


def shards(
    tokens,
    pre_gain,
    rate_factor,
    w_rec_in,
    w_rec_gate,
    conv_taps,
    rate_maps,
    input_maps,
    decay_param,
    w_query,
    w_latent,
    w_rope_key,
    latent_gain,
    w_expand,
    rec_gain,
    att_gain,
    w_out_rec,
    w_out_att,
    post_gain,
):
    row_count = tokens.shape[0]
    model_width = w_rec_in.shape[0]
    channels = w_rec_in.shape[1]
    heads_here = w_query.shape[1] // (NOPE + ROPE)
    group_size = lax.axis_size("tp")
    first_place = lax.axis_index("sp") * row_count
    places = first_place + jnp.arange(row_count)
    last_place = first_place + row_count - 1
    piece_wide = lax.all_gather(tokens, "tp", axis=1, tiled=True).astype(jnp.float32)
    piece_low = (piece_wide * pre_gain).astype(jnp.bfloat16)

    def accumulate(source, weight):
        return jnp.dot(source, weight, preferred_element_type=jnp.float32)

    squares = jnp.sum(piece_wide * piece_wide, axis=1, keepdims=True)
    sum_input = accumulate(piece_low, w_rec_in)
    sum_gate = accumulate(piece_low, w_rec_gate)
    sum_query = accumulate(piece_low, w_query)
    sum_latent = accumulate(piece_low, w_latent)
    sum_rope = accumulate(piece_low, w_rope_key)
    inverse = lax.rsqrt(squares / model_width + EPS)
    rec_input = (inverse * sum_input).astype(jnp.bfloat16)
    gate_value = inverse * sum_gate
    query_raw = inverse * sum_query
    latent_raw = inverse * sum_latent
    rope_raw = inverse * sum_rope
    rec_out, rec_squares = recurrent(
        rec_input,
        conv_taps,
        rate_maps,
        input_maps,
        jax.nn.softplus(-decay_param)[None, :],
        rate_factor[:, None],
        gate_value,
    )
    cosine, sine_part = angles(row_count, first_place, ROPE)
    query_heads = query_raw.reshape(row_count, heads_here, NOPE + ROPE)
    query_nope = query_heads[:, :, :NOPE].astype(jnp.bfloat16)
    query_rope = rotate(query_heads[:, :, NOPE:], cosine[:, None, :], sine_part[:, None, :]).astype(
        jnp.bfloat16
    )
    own_latent = (latent_raw * rms_inverse(latent_raw) * latent_gain).astype(jnp.bfloat16)
    rope_key = rotate(rope_raw, cosine, sine_part).astype(jnp.bfloat16)
    start_state = (
        jnp.full((heads_here, row_count), -jnp.inf, jnp.float32),
        jnp.zeros((heads_here, row_count), jnp.float32),
        jnp.zeros((heads_here, row_count, VDIM), jnp.float32),
    )
    expanded_local = jnp.dot(own_latent, w_expand, preferred_element_type=jnp.float32).astype(
        jnp.bfloat16
    )
    key_source = lax.all_gather(expanded_local, "sp", axis=0, tiled=True)
    rope_source = lax.all_gather(rope_key, "sp", axis=0, tiled=True)
    total_rows = key_source.shape[0]
    key_span = math.gcd(total_rows, span_limit)

    def one_span(span_index, state_inner):
        key_root = span_index * key_span

        def compute(state_deep):
            source_rows = lax.dynamic_slice_in_dim(key_source, span_index * key_span, key_span, 0)
            rope_rows = lax.dynamic_slice_in_dim(rope_source, span_index * key_span, key_span, 0)
            expanded = source_rows
            expanded = expanded.reshape(key_span, heads_here, NOPE + VDIM)
            return attend_block(
                state_deep,
                query_nope,
                query_rope,
                places,
                expanded[:, :, :NOPE],
                rope_rows,
                expanded[:, :, NOPE:],
                key_root,
            )

        def keep_state(state_deep):
            return state_deep

        return lax.cond(key_root <= last_place, compute, keep_state, state_inner)

    maxima, totals, accumulated = lax.fori_loop(0, total_rows // key_span, one_span, start_state)
    att_out = (
        (accumulated / totals[..., None]).transpose(1, 0, 2).reshape(row_count, heads_here * VDIM)
    )
    att_squares = jnp.sum(att_out * att_out, axis=1, keepdims=True)
    rec_total, att_total = lax.psum((rec_squares, att_squares), "tp")
    rec_norm = (rec_out * lax.rsqrt(rec_total / (channels * group_size) + EPS) * rec_gain).astype(
        jnp.bfloat16
    )
    att_norm = (
        att_out * lax.rsqrt(att_total / (heads_here * VDIM * group_size) + EPS) * att_gain
    ).astype(jnp.bfloat16)
    mixed_sum = lax.psum_scatter(
        (
            jnp.dot(rec_norm, w_out_rec, preferred_element_type=jnp.float32)
            + jnp.dot(att_norm, w_out_att, preferred_element_type=jnp.float32)
        ).astype(jnp.bfloat16),
        "tp",
        scatter_dimension=0,
        tiled=True,
    ).astype(jnp.float32)
    return (mixed_sum * rms_inverse(mixed_sum) * post_gain).astype(jnp.bfloat16)


def solution(mesh):
    placed = (
        P("sp", "tp"),
        P(),
        P("sp"),
        P(None, "tp"),
        P(None, "tp"),
        P(None, "tp"),
        P("tp", None, None),
        P("tp", None, None),
        P("tp"),
        P(None, "tp"),
        P(),
        P(),
        P(),
        P(None, "tp"),
        P("tp"),
        P("tp"),
        P("tp", None),
        P("tp", None),
        P(),
    )
    return jax.shard_map(
        shards, mesh=mesh, in_specs=placed, out_specs=P(("sp", "tp"), None), check_vma=False
    )
```

```python
import functools
import math

import jax
import jax.numpy as jnp
from jax import lax
from jax.experimental import pallas as pl
from jax.experimental.pallas import tpu as pltpu
from jax.sharding import PartitionSpec as P

NOPE = 128
ROPE = 64
VDIM = 128


EPS = 1e-06
RATE_C = 8.0
THETA = 10000.0
span_limit = 2048


def passed_along(block, axis, distance):
    devices = range(lax.axis_size(axis))
    route = [(i - distance, i) for i in devices if i - distance in devices]
    return lax.ppermute(block, axis, route)


def entering(value, axis, join, neutral):
    count, mine = (lax.axis_size(axis), lax.axis_index(axis))
    pieces = jax.tree.map(lambda part: lax.all_gather(part, axis), value)
    subtotal = jax.tree.map(
        lambda part, zero: jnp.full_like(part, 0) + jnp.asarray(zero, part.dtype), value, neutral
    )

    def step(position, subtotal):
        longer = join(subtotal, jax.tree.map(lambda part: part[position], pieces))
        return jax.tree.map(lambda new, old: jnp.where(position < mine, new, old), longer, subtotal)

    return lax.fori_loop(0, count - 1, step, subtotal)


def rms_inverse(values):
    return lax.rsqrt(jnp.mean(values * values, axis=-1, keepdims=True) + EPS)


def rotate(values, cosine, sine_part):
    half_width = values.shape[-1] // 2
    leading = values[..., :half_width]
    trailing = values[..., half_width:]
    return jnp.concatenate(
        [leading * cosine - trailing * sine_part, trailing * cosine + leading * sine_part], axis=-1
    )


def angles(length, offset, span_width):
    frequency = 1.0 / THETA ** (jnp.arange(0, span_width, 2).astype(jnp.float32) / span_width)
    places = (offset + jnp.arange(length)).astype(jnp.float32)
    turned = places[:, None] * frequency[None, :]
    return (jnp.cos(turned), jnp.sin(turned))


def combine_steps(earlier, later):
    return (earlier[0] * later[0], later[0] * earlier[1] + later[1])


def attend_block(state_now, query_nope, query_rope, places, keys_nope, key_rope, values, key_root):
    maxima, totals, accumulated = state_now
    scaling = 1.0 / math.sqrt(query_nope.shape[-1] + query_rope.shape[-1])
    scores = jnp.einsum("qhd,khd->hqk", query_nope, keys_nope, preferred_element_type=jnp.float32)
    scores = scores + jnp.einsum(
        "qhd,kd->hqk", query_rope, key_rope, preferred_element_type=jnp.float32
    )
    scores = scores * scaling
    key_places = key_root + jnp.arange(keys_nope.shape[0])
    visible = key_places[None, :] <= places[:, None]
    scores = jnp.where(visible[None], scores, -jnp.inf)
    largest = jnp.maximum(maxima, jnp.max(scores, axis=-1))
    anchor = jnp.where(largest == -jnp.inf, 0.0, largest)
    weights = jnp.exp(scores - anchor[..., None])
    shrink = jnp.exp(maxima - anchor)
    totals = totals * shrink + jnp.sum(weights, axis=-1)
    accumulated = accumulated * shrink[..., None] + jnp.einsum(
        "hqk,khd->hqd", weights.astype(jnp.bfloat16), values, preferred_element_type=jnp.float32
    )
    return (largest, totals, accumulated)


MESH = pl.DeviceIdType.MESH


def one_minus_exp(y):
    series = 1.0 + y * (1.0 / 8.0)
    for order in (7, 6, 5, 4, 3, 2):
        series = 1.0 + y * (1.0 / order) * series
    return jnp.where(y > -0.5, -y * series, 1.0 - jnp.exp(y))


def gelu_tanh(x):
    inner = math.sqrt(2.0 / math.pi) * (x + 0.044715 * (x * x * x))
    return 0.5 * x * (1.0 + jnp.tanh(inner))


def rec_kernel(
    n, rec_ref, taps_ref, rmap_ref, imap_ref, soft_ref, rate_ref, gate_ref,
    out_ref, padded, tail_tx, tail_rx, carry_tx, carry_rx, sems, rsems,
):
    me = lax.axis_index("sp")
    rows, channels = rec_ref.shape
    barrier = pltpu.get_barrier_semaphore()
    for d in range(1, n):
        pl.semaphore_signal(
            barrier, inc=1, device_id={"sp": lax.rem(me + d, n)}, device_id_type=MESH
        )
    x = rec_ref[...].astype(jnp.float32)
    tail_tx[...] = x[rows - 8 :, :]
    padded[8:, :] = x
    pl.semaphore_wait(barrier, n - 1)
    tail = pltpu.make_async_remote_copy(
        src_ref=tail_tx, dst_ref=tail_rx, send_sem=sems.at[0], recv_sem=rsems.at[0],
        device_id={"sp": lax.rem(me + 1, n)}, device_id_type=MESH,
    )
    tail.start()
    tail.wait()
    padded[0:8, :] = jnp.where(me > 0, tail_rx[...], 0.0)
    count = taps_ref.shape[0]
    conv = taps_ref[0:1, :] * padded[9 - count : 9 - count + rows, :]
    for k in range(1, count):
        conv = conv + taps_ref[k : k + 1, :] * padded[9 - count + k : 9 - count + k + rows, :]
    low = conv.astype(jnp.bfloat16)
    width = rmap_ref.shape[1]
    rate, entry = [], []
    for b in range(rmap_ref.shape[0]):
        part = low[:, b * width : (b + 1) * width]
        rate.append(jnp.dot(part, rmap_ref[b], preferred_element_type=jnp.float32))
        entry.append(jnp.dot(part, imap_ref[b], preferred_element_type=jnp.float32))
    rate = jax.nn.sigmoid(jnp.concatenate(rate, axis=1))
    entry = jax.nn.sigmoid(jnp.concatenate(entry, axis=1))
    log_keep = -RATE_C * rate_ref[...] * rate * soft_ref[...]
    a = jnp.exp(log_keep)
    b = jnp.sqrt(one_minus_exp(2.0 * log_keep)) * entry * conv
    row = lax.broadcasted_iota(jnp.int32, (rows, channels), 0)
    d = 1
    while d < rows:
        inside = row >= d
        b = a * jnp.where(inside, pltpu.roll(b, d, 0), 0.0) + b
        a = a * jnp.where(inside, pltpu.roll(a, d, 0), 1.0)
        d *= 2
    carry_tx[...] = jnp.zeros_like(carry_tx)
    carry_tx[0:1, :] = a[rows - 1 :, :]
    carry_tx[1:2, :] = b[rows - 1 :, :]
    copies = []
    for d in range(1, n):
        copies.append(
            pltpu.make_async_remote_copy(
                src_ref=carry_tx, dst_ref=carry_rx.at[me], send_sem=sems.at[d],
                recv_sem=rsems.at[d], device_id={"sp": lax.rem(me + d, n)}, device_id_type=MESH,
            )
        )
        copies[-1].start()
    gated = gelu_tanh(gate_ref[...])
    for copy in copies:
        copy.wait()
    carried = jnp.zeros((1, channels), jnp.float32)
    for s in range(n - 1):
        longer = carry_rx[s, 0:1, :] * carried + carry_rx[s, 1:2, :]
        carried = jnp.where(s < me, longer, carried)
    rec_out = (b + a * carried) * gated
    out_ref[...] = rec_out


def recurrent(rec_input, conv_taps, rate_maps, input_maps, soft, rate, gate_value):
    n = lax.axis_size("sp")
    rows, channels = rec_input.shape
    vmem = pl.BlockSpec(memory_space=pltpu.VMEM)
    return pl.pallas_call(
        functools.partial(rec_kernel, n),
        out_shape=jax.ShapeDtypeStruct((rows, channels), jnp.float32),
        in_specs=[vmem] * 7,
        out_specs=vmem,
        scratch_shapes=[
            pltpu.VMEM((rows + 8, channels), jnp.float32),
            pltpu.VMEM((8, channels), jnp.float32),
            pltpu.VMEM((8, channels), jnp.float32),
            pltpu.VMEM((8, channels), jnp.float32),
            pltpu.VMEM((n, 8, channels), jnp.float32),
            pltpu.SemaphoreType.DMA((n,)),
            pltpu.SemaphoreType.DMA((n,)),
        ],
        compiler_params=pltpu.CompilerParams(collective_id=0, has_side_effects=True),
        cost_estimate=pl.CostEstimate(flops=20_000_000, bytes_accessed=2_000_000, transcendentals=0),
        name="recurrent",
    )(rec_input, conv_taps, rate_maps, input_maps, soft, rate, gate_value)


def out_kernel(
    n, rec_ref, att_ref, rgain_ref, again_ref, wrec_ref, watt_ref, post_ref, out_ref,
    rec_norm, att_norm, sq_tx, sq_rx, part, rx1, tx2, rx2, mixed,
    sq_s, sq_r, s1, r1, s2, r2,
):
    me = lax.axis_index("tp")
    core, group = lax.rem(me, 2), me // 2
    groups = n // 2
    rows = rec_ref.shape[0]
    chunks, _, _, block, cols = part.shape
    barrier = pltpu.get_barrier_semaphore()
    for d in range(1, n):
        pl.semaphore_signal(
            barrier, inc=1, device_id={"tp": lax.rem(me + d, n)}, device_id_type=MESH
        )

    def row_squares(ref):
        x = ref[...]
        ones = jnp.ones((8, x.shape[1]), jnp.float32)
        return lax.dot_general(
            ones, x * x, (((1,), (1,)), ((), ())),
            precision=lax.Precision.HIGHEST, preferred_element_type=jnp.float32,
        )

    which = lax.broadcasted_iota(jnp.int32, (8, rows), 0)
    sq_tx[...] = jnp.where(which < 4, row_squares(rec_ref), row_squares(att_ref))
    pl.semaphore_wait(barrier, n - 1)
    copies = []
    for d in range(1, n):
        copies.append(
            pltpu.make_async_remote_copy(
                src_ref=sq_tx, dst_ref=sq_rx.at[d - 1], send_sem=sq_s.at[d - 1],
                recv_sem=sq_r.at[d - 1], device_id={"tp": lax.rem(me + d, n)},
                device_id_type=MESH,
            )
        )
        copies[-1].start()
    total = sq_tx[...]
    for d in range(1, n):
        copies[d - 1].wait()
        total = total + sq_rx[d - 1]
    total = jnp.transpose(total)
    rec_inv = lax.rsqrt(total[:, 0:1] / (rec_ref.shape[1] * n) + EPS)
    att_inv = lax.rsqrt(total[:, 4:5] / (att_ref.shape[1] * n) + EPS)
    rec_norm[...] = (rec_ref[...] * rec_inv * rgain_ref[...]).astype(jnp.bfloat16)
    att_norm[...] = (att_ref[...] * att_inv * again_ref[...]).astype(jnp.bfloat16)
    partner = group * 2 + (1 - core)
    first, second = [], []

    def cross(k):
        first[k].wait()
        pair = part[k, core].astype(jnp.float32) + rx1[k].astype(jnp.float32)
        tx2[k] = pair.astype(jnp.bfloat16)
        for e in range(1, groups):
            other = lax.rem(group + e, groups)
            second.append(
                pltpu.make_async_remote_copy(
                    src_ref=tx2.at[k, other], dst_ref=rx2.at[k, e - 1],
                    send_sem=s2.at[k, e - 1], recv_sem=r2.at[k, e - 1],
                    device_id={"tp": other * 2 + core}, device_id_type=MESH,
                )
            )
            second[-1].start()

    step = min(cols, 256)
    for k in range(chunks):
        for at in range(0, cols, step):
            here = slice(k * cols + at, k * cols + at + step)
            piece = (
                jnp.dot(rec_norm[...], wrec_ref[:, here], preferred_element_type=jnp.float32)
                + jnp.dot(att_norm[...], watt_ref[:, here], preferred_element_type=jnp.float32)
            ).astype(jnp.bfloat16)
            for j in range(n):
                part[k, j % 2, j // 2, :, at : at + step] = piece[j * block : (j + 1) * block]
        first.append(
            pltpu.make_async_remote_copy(
                src_ref=part.at[k, 1 - core], dst_ref=rx1.at[k], send_sem=s1.at[k],
                recv_sem=r1.at[k], device_id={"tp": partner}, device_id_type=MESH,
            )
        )
        first[-1].start()
        if k > 0:
            cross(k - 1)
    cross(chunks - 1)
    squares = jnp.zeros((block, 1), jnp.float32)
    for k in range(chunks):
        value = tx2[k, group].astype(jnp.float32)
        for e in range(1, groups):
            second[k * (groups - 1) + e - 1].wait()
            value = value + rx2[k, e - 1].astype(jnp.float32)
        mixed[k] = value
        squares = squares + jnp.sum(value * value, axis=1, keepdims=True)
    inverse = lax.rsqrt(squares / (chunks * cols) + EPS)
    for k in range(chunks):
        here = slice(k * cols, (k + 1) * cols)
        out_ref[:, here] = (mixed[k] * inverse * post_ref[:, here]).astype(jnp.bfloat16)


def project_out(rec_out, att_out, rec_gain, att_gain, w_out_rec, w_out_att, post_gain):
    n = lax.axis_size("tp")
    rows, channels = rec_out.shape
    width = w_out_rec.shape[1]
    chunks = math.gcd(width // 128, 4)
    cols, block, groups = width // chunks, rows // n, n // 2
    vmem = pl.BlockSpec(memory_space=pltpu.VMEM)
    low, dma = jnp.bfloat16, pltpu.SemaphoreType.DMA
    far = max(groups - 1, 1)
    return pl.pallas_call(
        functools.partial(out_kernel, n),
        out_shape=jax.ShapeDtypeStruct((block, width), low),
        in_specs=[vmem] * 7,
        out_specs=vmem,
        scratch_shapes=[
            pltpu.VMEM((rows, channels), low),
            pltpu.VMEM(att_out.shape, low),
            pltpu.VMEM((8, rows), jnp.float32),
            pltpu.VMEM((n - 1, 8, rows), jnp.float32),
            pltpu.VMEM((chunks, 2, groups, block, cols), low),
            pltpu.VMEM((chunks, groups, block, cols), low),
            pltpu.VMEM((chunks, groups, block, cols), low),
            pltpu.VMEM((chunks, far, block, cols), low),
            pltpu.VMEM((chunks, block, cols), jnp.float32),
            dma((n - 1,)),
            dma((n - 1,)),
            dma((chunks,)),
            dma((chunks,)),
            dma((chunks, far)),
            dma((chunks, far)),
        ],
        compiler_params=pltpu.CompilerParams(collective_id=1, has_side_effects=True),
        cost_estimate=pl.CostEstimate(
            flops=4 * rows * channels * width, bytes_accessed=8_000_000, transcendentals=0
        ),
        name="project_out",
    )(rec_out, att_out, rec_gain[None, :], att_gain[None, :], w_out_rec, w_out_att, post_gain[None, :])


def shards(
    tokens,
    pre_gain,
    rate_factor,
    w_rec_in,
    w_rec_gate,
    conv_taps,
    rate_maps,
    input_maps,
    decay_param,
    w_query,
    w_latent,
    w_rope_key,
    latent_gain,
    w_expand,
    rec_gain,
    att_gain,
    w_out_rec,
    w_out_att,
    post_gain,
):
    row_count = tokens.shape[0]
    model_width = w_rec_in.shape[0]
    heads_here = w_query.shape[1] // (NOPE + ROPE)
    first_place = lax.axis_index("sp") * row_count
    places = first_place + jnp.arange(row_count)
    last_place = first_place + row_count - 1
    piece_wide = lax.all_gather(tokens, "tp", axis=1, tiled=True).astype(jnp.float32)
    piece_low = (piece_wide * pre_gain).astype(jnp.bfloat16)

    def accumulate(source, weight):
        return jnp.dot(source, weight, preferred_element_type=jnp.float32)

    squares = jnp.sum(piece_wide * piece_wide, axis=1, keepdims=True)
    sum_input = accumulate(piece_low, w_rec_in)
    sum_gate = accumulate(piece_low, w_rec_gate)
    sum_query = accumulate(piece_low, w_query)
    sum_latent = accumulate(piece_low, w_latent)
    sum_rope = accumulate(piece_low, w_rope_key)
    inverse = lax.rsqrt(squares / model_width + EPS)
    rec_input = (inverse * sum_input).astype(jnp.bfloat16)
    gate_value = inverse * sum_gate
    query_raw = inverse * sum_query
    latent_raw = inverse * sum_latent
    rope_raw = inverse * sum_rope
    rec_out = recurrent(
        rec_input,
        conv_taps,
        rate_maps,
        input_maps,
        jax.nn.softplus(-decay_param)[None, :],
        rate_factor[:, None],
        gate_value,
    )
    cosine, sine_part = angles(row_count, first_place, ROPE)
    query_heads = query_raw.reshape(row_count, heads_here, NOPE + ROPE)
    query_nope = query_heads[:, :, :NOPE].astype(jnp.bfloat16)
    query_rope = rotate(query_heads[:, :, NOPE:], cosine[:, None, :], sine_part[:, None, :]).astype(
        jnp.bfloat16
    )
    own_latent = (latent_raw * rms_inverse(latent_raw) * latent_gain).astype(jnp.bfloat16)
    rope_key = rotate(rope_raw, cosine, sine_part).astype(jnp.bfloat16)
    start_state = (
        jnp.full((heads_here, row_count), -jnp.inf, jnp.float32),
        jnp.zeros((heads_here, row_count), jnp.float32),
        jnp.zeros((heads_here, row_count, VDIM), jnp.float32),
    )
    expanded_local = jnp.dot(own_latent, w_expand, preferred_element_type=jnp.float32).astype(
        jnp.bfloat16
    )
    key_source = lax.all_gather(expanded_local, "sp", axis=0, tiled=True)
    rope_source = lax.all_gather(rope_key, "sp", axis=0, tiled=True)
    total_rows = key_source.shape[0]
    key_span = math.gcd(total_rows, span_limit)

    def one_span(span_index, state_inner):
        key_root = span_index * key_span

        def compute(state_deep):
            source_rows = lax.dynamic_slice_in_dim(key_source, span_index * key_span, key_span, 0)
            rope_rows = lax.dynamic_slice_in_dim(rope_source, span_index * key_span, key_span, 0)
            expanded = source_rows
            expanded = expanded.reshape(key_span, heads_here, NOPE + VDIM)
            return attend_block(
                state_deep,
                query_nope,
                query_rope,
                places,
                expanded[:, :, :NOPE],
                rope_rows,
                expanded[:, :, NOPE:],
                key_root,
            )

        def keep_state(state_deep):
            return state_deep

        return lax.cond(key_root <= last_place, compute, keep_state, state_inner)

    maxima, totals, accumulated = lax.fori_loop(0, total_rows // key_span, one_span, start_state)
    att_out = (
        (accumulated / totals[..., None]).transpose(1, 0, 2).reshape(row_count, heads_here * VDIM)
    )
    return project_out(rec_out, att_out, rec_gain, att_gain, w_out_rec, w_out_att, post_gain)


def solution(mesh):
    placed = (
        P("sp", "tp"),
        P(),
        P("sp"),
        P(None, "tp"),
        P(None, "tp"),
        P(None, "tp"),
        P("tp", None, None),
        P("tp", None, None),
        P("tp"),
        P(None, "tp"),
        P(),
        P(),
        P(),
        P(None, "tp"),
        P("tp"),
        P("tp"),
        P("tp", None),
        P("tp", None),
        P(),
    )
    return jax.shard_map(
        shards, mesh=mesh, in_specs=placed, out_specs=P(("sp", "tp"), None), check_vma=False
    )
```

```python
import functools
import math

import jax
import jax.numpy as jnp
from jax import lax
from jax.experimental import pallas as pl
from jax.experimental.pallas import tpu as pltpu
from jax.sharding import PartitionSpec as P

NOPE = 128
ROPE = 64
VDIM = 128


EPS = 1e-06
RATE_C = 8.0
THETA = 10000.0


def rms_inverse(values):
    return lax.rsqrt(jnp.mean(values * values, axis=-1, keepdims=True) + EPS)


def rotate(values, cosine, sine_part):
    half_width = values.shape[-1] // 2
    leading = values[..., :half_width]
    trailing = values[..., half_width:]
    return jnp.concatenate(
        [leading * cosine - trailing * sine_part, trailing * cosine + leading * sine_part], axis=-1
    )


def angles(length, offset, span_width):
    frequency = 1.0 / THETA ** (jnp.arange(0, span_width, 2).astype(jnp.float32) / span_width)
    places = (offset + jnp.arange(length)).astype(jnp.float32)
    turned = places[:, None] * frequency[None, :]
    return (jnp.cos(turned), jnp.sin(turned))


MESH = pl.DeviceIdType.MESH


def one_minus_exp(y):
    series = 1.0 + y * (1.0 / 8.0)
    for order in (7, 6, 5, 4, 3, 2):
        series = 1.0 + y * (1.0 / order) * series
    return jnp.where(y > -0.5, -y * series, 1.0 - jnp.exp(y))


def gelu_tanh(x):
    inner = math.sqrt(2.0 / math.pi) * (x + 0.044715 * (x * x * x))
    return 0.5 * x * (1.0 + jnp.tanh(inner))


def rec_kernel(
    n, rec_ref, taps_ref, rmap_ref, imap_ref, soft_ref, rate_ref, gate_ref,
    out_ref, padded, tail_tx, tail_rx, carry_tx, carry_rx, sems, rsems,
):
    me = lax.axis_index("sp")
    rows, channels = rec_ref.shape
    barrier = pltpu.get_barrier_semaphore()
    for d in range(1, n):
        pl.semaphore_signal(
            barrier, inc=1, device_id={"sp": lax.rem(me + d, n)}, device_id_type=MESH
        )
    x = rec_ref[...].astype(jnp.float32)
    tail_tx[...] = x[rows - 8 :, :]
    padded[8:, :] = x
    pl.semaphore_wait(barrier, n - 1)
    tail = pltpu.make_async_remote_copy(
        src_ref=tail_tx, dst_ref=tail_rx, send_sem=sems.at[0], recv_sem=rsems.at[0],
        device_id={"sp": lax.rem(me + 1, n)}, device_id_type=MESH,
    )
    tail.start()
    tail.wait()
    padded[0:8, :] = jnp.where(me > 0, tail_rx[...], 0.0)
    count = taps_ref.shape[0]
    conv = taps_ref[0:1, :] * padded[9 - count : 9 - count + rows, :]
    for k in range(1, count):
        conv = conv + taps_ref[k : k + 1, :] * padded[9 - count + k : 9 - count + k + rows, :]
    low = conv.astype(jnp.bfloat16)
    width = rmap_ref.shape[1]
    rate, entry = [], []
    for b in range(rmap_ref.shape[0]):
        part = low[:, b * width : (b + 1) * width]
        rate.append(jnp.dot(part, rmap_ref[b], preferred_element_type=jnp.float32))
        entry.append(jnp.dot(part, imap_ref[b], preferred_element_type=jnp.float32))
    rate = jax.nn.sigmoid(jnp.concatenate(rate, axis=1))
    entry = jax.nn.sigmoid(jnp.concatenate(entry, axis=1))
    log_keep = -RATE_C * rate_ref[...] * rate * soft_ref[...]
    a = jnp.exp(log_keep)
    b = jnp.sqrt(one_minus_exp(2.0 * log_keep)) * entry * conv
    row = lax.broadcasted_iota(jnp.int32, (rows, channels), 0)
    d = 1
    while d < rows:
        inside = row >= d
        b = a * jnp.where(inside, pltpu.roll(b, d, 0), 0.0) + b
        a = a * jnp.where(inside, pltpu.roll(a, d, 0), 1.0)
        d *= 2
    carry_tx[...] = jnp.zeros_like(carry_tx)
    carry_tx[0:1, :] = a[rows - 1 :, :]
    carry_tx[1:2, :] = b[rows - 1 :, :]
    copies = []
    for d in range(1, n):
        copies.append(
            pltpu.make_async_remote_copy(
                src_ref=carry_tx, dst_ref=carry_rx.at[me], send_sem=sems.at[d],
                recv_sem=rsems.at[d], device_id={"sp": lax.rem(me + d, n)}, device_id_type=MESH,
            )
        )
        copies[-1].start()
    gated = gelu_tanh(gate_ref[...])
    for copy in copies:
        copy.wait()
    carried = jnp.zeros((1, channels), jnp.float32)
    for s in range(n - 1):
        longer = carry_rx[s, 0:1, :] * carried + carry_rx[s, 1:2, :]
        carried = jnp.where(s < me, longer, carried)
    rec_out = (b + a * carried) * gated
    out_ref[...] = rec_out


def recurrent(rec_input, conv_taps, rate_maps, input_maps, soft, rate, gate_value):
    n = lax.axis_size("sp")
    rows, channels = rec_input.shape
    vmem = pl.BlockSpec(memory_space=pltpu.VMEM)
    return pl.pallas_call(
        functools.partial(rec_kernel, n),
        out_shape=jax.ShapeDtypeStruct((rows, channels), jnp.float32),
        in_specs=[vmem] * 7,
        out_specs=vmem,
        scratch_shapes=[
            pltpu.VMEM((rows + 8, channels), jnp.float32),
            pltpu.VMEM((8, channels), jnp.float32),
            pltpu.VMEM((8, channels), jnp.float32),
            pltpu.VMEM((8, channels), jnp.float32),
            pltpu.VMEM((n, 8, channels), jnp.float32),
            pltpu.SemaphoreType.DMA((n,)),
            pltpu.SemaphoreType.DMA((n,)),
        ],
        compiler_params=pltpu.CompilerParams(collective_id=0, has_side_effects=True),
        cost_estimate=pl.CostEstimate(flops=20_000_000, bytes_accessed=2_000_000, transcendentals=0),
        name="recurrent",
    )(rec_input, conv_taps, rate_maps, input_maps, soft, rate, gate_value)


def out_kernel(
    n, rec_ref, att_ref, rgain_ref, again_ref, wrec_ref, watt_ref, post_ref, out_ref,
    rec_norm, att_norm, sq_tx, sq_rx, part, rx1, tx2, rx2, mixed,
    sq_s, sq_r, s1, r1, s2, r2,
):
    me = lax.axis_index("tp")
    core, group = lax.rem(me, 2), me // 2
    groups = n // 2
    rows = rec_ref.shape[0]
    chunks, _, _, block, cols = part.shape
    barrier = pltpu.get_barrier_semaphore()
    for d in range(1, n):
        pl.semaphore_signal(
            barrier, inc=1, device_id={"tp": lax.rem(me + d, n)}, device_id_type=MESH
        )

    def row_squares(ref):
        x = ref[...]
        ones = jnp.ones((8, x.shape[1]), jnp.float32)
        return lax.dot_general(
            ones, x * x, (((1,), (1,)), ((), ())),
            precision=lax.Precision.HIGHEST, preferred_element_type=jnp.float32,
        )

    which = lax.broadcasted_iota(jnp.int32, (8, rows), 0)
    sq_tx[...] = jnp.where(which < 4, row_squares(rec_ref), row_squares(att_ref))
    pl.semaphore_wait(barrier, n - 1)
    copies = []
    for d in range(1, n):
        copies.append(
            pltpu.make_async_remote_copy(
                src_ref=sq_tx, dst_ref=sq_rx.at[d - 1], send_sem=sq_s.at[d - 1],
                recv_sem=sq_r.at[d - 1], device_id={"tp": lax.rem(me + d, n)},
                device_id_type=MESH,
            )
        )
        copies[-1].start()
    total = sq_tx[...]
    for d in range(1, n):
        copies[d - 1].wait()
        total = total + sq_rx[d - 1]
    total = jnp.transpose(total)
    rec_inv = lax.rsqrt(total[:, 0:1] / (rec_ref.shape[1] * n) + EPS)
    att_inv = lax.rsqrt(total[:, 4:5] / (att_ref.shape[1] * n) + EPS)
    rec_norm[...] = (rec_ref[...] * rec_inv * rgain_ref[...]).astype(jnp.bfloat16)
    att_norm[...] = (att_ref[...] * att_inv * again_ref[...]).astype(jnp.bfloat16)
    partner = group * 2 + (1 - core)
    first, second = [], []

    def cross(k):
        first[k].wait()
        pair = part[k, core].astype(jnp.float32) + rx1[k].astype(jnp.float32)
        tx2[k] = pair.astype(jnp.bfloat16)
        for e in range(1, groups):
            other = lax.rem(group + e, groups)
            second.append(
                pltpu.make_async_remote_copy(
                    src_ref=tx2.at[k, other], dst_ref=rx2.at[k, e - 1],
                    send_sem=s2.at[k, e - 1], recv_sem=r2.at[k, e - 1],
                    device_id={"tp": other * 2 + core}, device_id_type=MESH,
                )
            )
            second[-1].start()

    step = min(cols, 256)
    for k in range(chunks):
        for at in range(0, cols, step):
            here = slice(k * cols + at, k * cols + at + step)
            piece = (
                jnp.dot(rec_norm[...], wrec_ref[:, here], preferred_element_type=jnp.float32)
                + jnp.dot(att_norm[...], watt_ref[:, here], preferred_element_type=jnp.float32)
            ).astype(jnp.bfloat16)
            for j in range(n):
                part[k, j % 2, j // 2, :, at : at + step] = piece[j * block : (j + 1) * block]
        first.append(
            pltpu.make_async_remote_copy(
                src_ref=part.at[k, 1 - core], dst_ref=rx1.at[k], send_sem=s1.at[k],
                recv_sem=r1.at[k], device_id={"tp": partner}, device_id_type=MESH,
            )
        )
        first[-1].start()
        if k > 0:
            cross(k - 1)
    cross(chunks - 1)
    squares = jnp.zeros((block, 1), jnp.float32)
    for k in range(chunks):
        value = tx2[k, group].astype(jnp.float32)
        for e in range(1, groups):
            second[k * (groups - 1) + e - 1].wait()
            value = value + rx2[k, e - 1].astype(jnp.float32)
        mixed[k] = value
        squares = squares + jnp.sum(value * value, axis=1, keepdims=True)
    inverse = lax.rsqrt(squares / (chunks * cols) + EPS)
    for k in range(chunks):
        here = slice(k * cols, (k + 1) * cols)
        out_ref[:, here] = (mixed[k] * inverse * post_ref[:, here]).astype(jnp.bfloat16)


def project_out(rec_out, att_out, rec_gain, att_gain, w_out_rec, w_out_att, post_gain):
    n = lax.axis_size("tp")
    rows, channels = rec_out.shape
    width = w_out_rec.shape[1]
    chunks = math.gcd(width // 128, 4)
    cols, block, groups = width // chunks, rows // n, n // 2
    vmem = pl.BlockSpec(memory_space=pltpu.VMEM)
    low, dma = jnp.bfloat16, pltpu.SemaphoreType.DMA
    far = max(groups - 1, 1)
    return pl.pallas_call(
        functools.partial(out_kernel, n),
        out_shape=jax.ShapeDtypeStruct((block, width), low),
        in_specs=[vmem] * 7,
        out_specs=vmem,
        scratch_shapes=[
            pltpu.VMEM((rows, channels), low),
            pltpu.VMEM(att_out.shape, low),
            pltpu.VMEM((8, rows), jnp.float32),
            pltpu.VMEM((n - 1, 8, rows), jnp.float32),
            pltpu.VMEM((chunks, 2, groups, block, cols), low),
            pltpu.VMEM((chunks, groups, block, cols), low),
            pltpu.VMEM((chunks, groups, block, cols), low),
            pltpu.VMEM((chunks, far, block, cols), low),
            pltpu.VMEM((chunks, block, cols), jnp.float32),
            dma((n - 1,)),
            dma((n - 1,)),
            dma((chunks,)),
            dma((chunks,)),
            dma((chunks, far)),
            dma((chunks, far)),
        ],
        compiler_params=pltpu.CompilerParams(collective_id=1, has_side_effects=True),
        cost_estimate=pl.CostEstimate(
            flops=4 * rows * channels * width, bytes_accessed=8_000_000, transcendentals=0
        ),
        name="project_out",
    )(rec_out, att_out, rec_gain[None, :], att_gain[None, :], w_out_rec, w_out_att, post_gain[None, :])


def attend_kernel(
    n, m, q_ref, lat_ref, wexp_ref, out_ref,
    buf, peak, total, accum, p_s, p_r, y_s, y_r, c_s, c_r,
):
    me, tp = lax.axis_index("sp"), lax.axis_index("tp")
    core, group, groups = lax.rem(tp, 2), tp // 2, m // 2
    partner = group * 2 + (1 - core)
    pieces, block, wide = lat_ref.shape
    rows = pieces * block
    latent = wexp_ref.shape[0]
    heads = wexp_ref.shape[1] // (NOPE + VDIM)
    scaling = 1.0 / math.sqrt(NOPE + ROPE)
    barrier = pltpu.get_barrier_semaphore()
    for d in range(1, n):
        pl.semaphore_signal(
            barrier, inc=1, device_id={"sp": lax.rem(me + d, n)}, device_id_type=MESH
        )
    for e in range(1, groups):
        pl.semaphore_signal(
            barrier, inc=1, device_id={"tp": lax.rem(group + e, groups) * 2 + core},
            device_id_type=MESH,
        )
    pl.semaphore_signal(barrier, inc=1, device_id={"tp": partner}, device_id_type=MESH)
    pl.semaphore_wait(barrier, n - 1 + groups)

    def ahead(d):
        return pltpu.make_async_remote_copy(
            src_ref=lat_ref.at[tp], dst_ref=buf.at[d, tp], send_sem=p_s.at[d], recv_sem=p_r.at[d],
            device_id={"sp": lax.rem(me + d, n)}, device_id_type=MESH,
        )

    def across(d, e):
        return pltpu.make_async_remote_copy(
            src_ref=buf.at[d, tp], dst_ref=buf.at[d, tp], send_sem=y_s.at[d, e],
            recv_sem=y_r.at[d, e], device_id={"tp": lax.rem(group + e, groups) * 2 + core},
            device_id_type=MESH,
        )

    def inside(d, e):
        piece = lax.rem(group - e + groups, groups) * 2 + core
        return pltpu.make_async_remote_copy(
            src_ref=buf.at[d, piece], dst_ref=buf.at[d, piece], send_sem=c_s.at[d, e],
            recv_sem=c_r.at[d, e], device_id={"tp": partner}, device_id_type=MESH,
        )

    def send_one(d, carry):
        @pl.when(me + d < n)
        def _():
            ahead(d).start()

        return carry

    lax.fori_loop(1, n, send_one, 0)

    def chunk(lat, own):
        expanded = jnp.dot(
            lat[:, :latent], wexp_ref[...], preferred_element_type=jnp.float32
        ).astype(jnp.bfloat16)
        key_rope = lat[:, latent:]
        for h in range(heads):
            base = h * (NOPE + VDIM)
            keys = jnp.concatenate([expanded[:, base : base + NOPE], key_rope], axis=1)
            width = keys.shape[1]
            scores = lax.dot_general(
                q_ref[:, h * width : (h + 1) * width], keys, (((1,), (1,)), ((), ())),
                preferred_element_type=jnp.float32,
            ) * scaling
            if own:
                at_row = lax.broadcasted_iota(jnp.int32, scores.shape, 0)
                at_col = lax.broadcasted_iota(jnp.int32, scores.shape, 1)
                scores = jnp.where(at_col <= at_row, scores, -jnp.inf)
            high = jnp.max(scores, axis=1, keepdims=True)
            if not own:
                high = jnp.maximum(high, peak[h])
            weights = jnp.exp(scores - high)
            added = jnp.sum(weights, axis=1, keepdims=True)
            mixed = jnp.dot(
                weights.astype(jnp.bfloat16), expanded[:, base + NOPE : base + NOPE + VDIM],
                preferred_element_type=jnp.float32,
            )
            if not own:
                shrink = jnp.exp(peak[h] - high)
                added = added + total[h] * shrink
                mixed = mixed + accum[h] * shrink
            peak[h] = high
            total[h] = added
            accum[h] = mixed

    chunk(lat_ref[...].reshape(rows, wide), True)

    def step(t, carry):
        @pl.when(t <= me)
        def _():
            ahead(t).wait_recv()
            for e in range(1, groups):
                across(t, e).start()
            inside(t, 0).start()

        @pl.when((t >= 2) & (t - 1 <= me))
        def _():
            for e in range(1, groups):
                across(t - 1, e).wait_recv()
                inside(t - 1, e).start()

        @pl.when((t >= 3) & (t - 2 <= me))
        def _():
            for e in range(groups):
                inside(t - 2, e).wait_recv()
            chunk(buf[t - 2].reshape(rows, wide), False)

        return carry

    lax.fori_loop(1, n + 2, step, 0)
    for h in range(heads):
        out_ref[:, h * VDIM : (h + 1) * VDIM] = accum[h] / total[h]

    def finish(d, carry):
        @pl.when(me + d < n)
        def _():
            ahead(d).wait_send()

        @pl.when(d <= me)
        def _():
            for e in range(1, groups):
                across(d, e).wait_send()
            for e in range(groups):
                inside(d, e).wait_send()

        return carry

    lax.fori_loop(1, n, finish, 0)


def attend(query, latent_rope, w_expand):
    n, m = lax.axis_size("sp"), lax.axis_size("tp")
    rows, wide = latent_rope.shape
    heads = w_expand.shape[1] // (NOPE + VDIM)
    vmem = pl.BlockSpec(memory_space=pltpu.VMEM)
    dma = pltpu.SemaphoreType.DMA
    block = rows // m
    return pl.pallas_call(
        functools.partial(attend_kernel, n, m),
        out_shape=jax.ShapeDtypeStruct((rows, heads * VDIM), jnp.float32),
        in_specs=[vmem] * 3,
        out_specs=vmem,
        scratch_shapes=[
            pltpu.VMEM((n, m, block, wide), jnp.bfloat16),
            pltpu.VMEM((heads, rows, 1), jnp.float32),
            pltpu.VMEM((heads, rows, 1), jnp.float32),
            pltpu.VMEM((heads, rows, VDIM), jnp.float32),
            dma((n,)),
            dma((n,)),
            dma((n, m // 2)),
            dma((n, m // 2)),
            dma((n, m // 2)),
            dma((n, m // 2)),
        ],
        compiler_params=pltpu.CompilerParams(collective_id=2, has_side_effects=True),
        cost_estimate=pl.CostEstimate(
            flops=2_000_000_000, bytes_accessed=4_000_000, transcendentals=0
        ),
        name="attend",
    )(query, latent_rope.reshape(m, block, wide), w_expand)


def shards(
    tokens,
    pre_gain,
    rate_factor,
    w_rec_in,
    w_rec_gate,
    conv_taps,
    rate_maps,
    input_maps,
    decay_param,
    w_query,
    w_latent,
    w_rope_key,
    latent_gain,
    w_expand,
    rec_gain,
    att_gain,
    w_out_rec,
    w_out_att,
    post_gain,
):
    row_count = tokens.shape[0]
    model_width = w_rec_in.shape[0]
    heads_here = w_query.shape[1] // (NOPE + ROPE)
    first_place = lax.axis_index("sp") * row_count
    piece_wide = lax.all_gather(tokens, "tp", axis=1, tiled=True).astype(jnp.float32)
    piece_low = (piece_wide * pre_gain).astype(jnp.bfloat16)

    def accumulate(source, weight):
        return jnp.dot(source, weight, preferred_element_type=jnp.float32)

    squares = jnp.sum(piece_wide * piece_wide, axis=1, keepdims=True)
    sum_input = accumulate(piece_low, w_rec_in)
    sum_gate = accumulate(piece_low, w_rec_gate)
    sum_query = accumulate(piece_low, w_query)
    sum_latent = accumulate(piece_low, w_latent)
    sum_rope = accumulate(piece_low, w_rope_key)
    inverse = lax.rsqrt(squares / model_width + EPS)
    rec_input = (inverse * sum_input).astype(jnp.bfloat16)
    gate_value = inverse * sum_gate
    query_raw = inverse * sum_query
    latent_raw = inverse * sum_latent
    rope_raw = inverse * sum_rope
    rec_out = recurrent(
        rec_input,
        conv_taps,
        rate_maps,
        input_maps,
        jax.nn.softplus(-decay_param)[None, :],
        rate_factor[:, None],
        gate_value,
    )
    cosine, sine_part = angles(row_count, first_place, ROPE)
    query_heads = query_raw.reshape(row_count, heads_here, NOPE + ROPE)
    low = jnp.bfloat16
    query_rope = rotate(query_heads[:, :, NOPE:], cosine[:, None, :], sine_part[:, None, :])
    fill = NOPE - ROPE
    query = jnp.concatenate(
        [query_heads[:, :, :NOPE], query_rope, jnp.zeros((row_count, heads_here, fill))], axis=-1
    ).astype(low)
    own_latent = (latent_raw * rms_inverse(latent_raw) * latent_gain).astype(low)
    rope_key = rotate(rope_raw, cosine, sine_part).astype(low)
    latent_rope = jnp.concatenate(
        [own_latent, rope_key, jnp.zeros((row_count, fill), low)], axis=-1
    )
    att_out = attend(query.reshape(row_count, heads_here * 2 * NOPE), latent_rope, w_expand)
    return project_out(rec_out, att_out, rec_gain, att_gain, w_out_rec, w_out_att, post_gain)


def solution(mesh):
    placed = (
        P("sp", "tp"),
        P(),
        P("sp"),
        P(None, "tp"),
        P(None, "tp"),
        P(None, "tp"),
        P("tp", None, None),
        P("tp", None, None),
        P("tp"),
        P(None, "tp"),
        P(),
        P(),
        P(),
        P(None, "tp"),
        P("tp"),
        P("tp"),
        P("tp", None),
        P("tp", None),
        P(),
    )
    return jax.shard_map(
        shards, mesh=mesh, in_specs=placed, out_specs=P(("sp", "tp"), None), check_vma=False
    )
```

```python
import functools
import math

import jax
import jax.numpy as jnp
from jax import lax
from jax.experimental import pallas as pl
from jax.experimental.pallas import tpu as pltpu
from jax.sharding import PartitionSpec as P

NOPE = 128
ROPE = 64
VDIM = 128


EPS = 1e-06
RATE_C = 8.0
THETA = 10000.0


def rotate(values, cosine, sine_part):
    half_width = values.shape[-1] // 2
    leading = values[..., :half_width]
    trailing = values[..., half_width:]
    return jnp.concatenate(
        [leading * cosine - trailing * sine_part, trailing * cosine + leading * sine_part], axis=-1
    )


def angles(length, offset, span_width):
    frequency = 1.0 / THETA ** (jnp.arange(0, span_width, 2).astype(jnp.float32) / span_width)
    places = (offset + jnp.arange(length)).astype(jnp.float32)
    turned = places[:, None] * frequency[None, :]
    return (jnp.cos(turned), jnp.sin(turned))


MESH = pl.DeviceIdType.MESH


def one_minus_exp(y):
    series = 1.0 + y * (1.0 / 8.0)
    for order in (7, 6, 5, 4, 3, 2):
        series = 1.0 + y * (1.0 / order) * series
    return jnp.where(y > -0.5, -y * series, 1.0 - jnp.exp(y))


def gelu_tanh(x):
    inner = math.sqrt(2.0 / math.pi) * (x + 0.044715 * (x * x * x))
    return 0.5 * x * (1.0 + jnp.tanh(inner))


def rec_kernel(
    n, rec_ref, taps_ref, rmap_ref, imap_ref, soft_ref, rate_ref, gate_ref,
    out_ref, padded, tail_tx, tail_rx, carry_tx, carry_rx, sems, rsems,
):
    me = lax.axis_index("sp")
    rows, channels = rec_ref.shape
    barrier = pltpu.get_barrier_semaphore()
    for d in range(1, n):
        pl.semaphore_signal(
            barrier, inc=1, device_id={"sp": lax.rem(me + d, n)}, device_id_type=MESH
        )
    x = rec_ref[...].astype(jnp.float32)
    tail_tx[...] = x[rows - 8 :, :]
    padded[8:, :] = x
    pl.semaphore_wait(barrier, n - 1)
    tail = pltpu.make_async_remote_copy(
        src_ref=tail_tx, dst_ref=tail_rx, send_sem=sems.at[0], recv_sem=rsems.at[0],
        device_id={"sp": lax.rem(me + 1, n)}, device_id_type=MESH,
    )
    tail.start()
    tail.wait()
    padded[0:8, :] = jnp.where(me > 0, tail_rx[...], 0.0)
    count = taps_ref.shape[0]
    conv = taps_ref[0:1, :] * padded[9 - count : 9 - count + rows, :]
    for k in range(1, count):
        conv = conv + taps_ref[k : k + 1, :] * padded[9 - count + k : 9 - count + k + rows, :]
    low = conv.astype(jnp.bfloat16)
    width = rmap_ref.shape[1]
    rate, entry = [], []
    for b in range(rmap_ref.shape[0]):
        part = low[:, b * width : (b + 1) * width]
        rate.append(jnp.dot(part, rmap_ref[b], preferred_element_type=jnp.float32))
        entry.append(jnp.dot(part, imap_ref[b], preferred_element_type=jnp.float32))
    rate = jax.nn.sigmoid(jnp.concatenate(rate, axis=1))
    entry = jax.nn.sigmoid(jnp.concatenate(entry, axis=1))
    log_keep = -RATE_C * rate_ref[...] * rate * soft_ref[...]
    a = jnp.exp(log_keep)
    b = jnp.sqrt(one_minus_exp(2.0 * log_keep)) * entry * conv
    row = lax.broadcasted_iota(jnp.int32, (rows, channels), 0)
    d = 1
    while d < rows:
        inside = row >= d
        b = a * jnp.where(inside, pltpu.roll(b, d, 0), 0.0) + b
        a = a * jnp.where(inside, pltpu.roll(a, d, 0), 1.0)
        d *= 2
    carry_tx[...] = jnp.zeros_like(carry_tx)
    carry_tx[0:1, :] = a[rows - 1 :, :]
    carry_tx[1:2, :] = b[rows - 1 :, :]
    copies = []
    for d in range(1, n):
        copies.append(
            pltpu.make_async_remote_copy(
                src_ref=carry_tx, dst_ref=carry_rx.at[me], send_sem=sems.at[d],
                recv_sem=rsems.at[d], device_id={"sp": lax.rem(me + d, n)}, device_id_type=MESH,
            )
        )
        copies[-1].start()
    gated = gelu_tanh(gate_ref[...])
    for copy in copies:
        copy.wait()
    carried = jnp.zeros((1, channels), jnp.float32)
    for s in range(n - 1):
        longer = carry_rx[s, 0:1, :] * carried + carry_rx[s, 1:2, :]
        carried = jnp.where(s < me, longer, carried)
    rec_out = (b + a * carried) * gated
    out_ref[...] = rec_out


def recurrent(rec_input, conv_taps, rate_maps, input_maps, soft, rate, gate_value):
    n = lax.axis_size("sp")
    rows, channels = rec_input.shape
    vmem = pl.BlockSpec(memory_space=pltpu.VMEM)
    return pl.pallas_call(
        functools.partial(rec_kernel, n),
        out_shape=jax.ShapeDtypeStruct((rows, channels), jnp.float32),
        in_specs=[vmem] * 7,
        out_specs=vmem,
        scratch_shapes=[
            pltpu.VMEM((rows + 8, channels), jnp.float32),
            pltpu.VMEM((8, channels), jnp.float32),
            pltpu.VMEM((8, channels), jnp.float32),
            pltpu.VMEM((8, channels), jnp.float32),
            pltpu.VMEM((n, 8, channels), jnp.float32),
            pltpu.SemaphoreType.DMA((n,)),
            pltpu.SemaphoreType.DMA((n,)),
        ],
        compiler_params=pltpu.CompilerParams(collective_id=0, has_side_effects=True),
        cost_estimate=pl.CostEstimate(flops=20_000_000, bytes_accessed=2_000_000, transcendentals=0),
        name="recurrent",
    )(rec_input, conv_taps, rate_maps, input_maps, soft, rate, gate_value)


def out_kernel(
    n, rec_ref, att_ref, rgain_ref, again_ref, wrec_ref, watt_ref, post_ref, out_ref,
    rec_norm, att_norm, sq_tx, sq_rx, part, rx1, tx2, rx2, mixed,
    sq_s, sq_r, s1, r1, s2, r2,
):
    me = lax.axis_index("tp")
    core, group = lax.rem(me, 2), me // 2
    groups = n // 2
    rows = rec_ref.shape[0]
    chunks, _, _, block, cols = part.shape
    barrier = pltpu.get_barrier_semaphore()
    for d in range(1, n):
        pl.semaphore_signal(
            barrier, inc=1, device_id={"tp": lax.rem(me + d, n)}, device_id_type=MESH
        )

    def row_squares(ref):
        x = ref[...]
        ones = jnp.ones((8, x.shape[1]), jnp.float32)
        return lax.dot_general(
            ones, x * x, (((1,), (1,)), ((), ())),
            precision=lax.Precision.HIGHEST, preferred_element_type=jnp.float32,
        )

    which = lax.broadcasted_iota(jnp.int32, (8, rows), 0)
    sq_tx[...] = jnp.where(which < 4, row_squares(rec_ref), row_squares(att_ref))
    pl.semaphore_wait(barrier, n - 1)
    copies = []
    for d in range(1, n):
        copies.append(
            pltpu.make_async_remote_copy(
                src_ref=sq_tx, dst_ref=sq_rx.at[d - 1], send_sem=sq_s.at[d - 1],
                recv_sem=sq_r.at[d - 1], device_id={"tp": lax.rem(me + d, n)},
                device_id_type=MESH,
            )
        )
        copies[-1].start()
    total = sq_tx[...]
    for d in range(1, n):
        copies[d - 1].wait()
        total = total + sq_rx[d - 1]
    total = jnp.transpose(total)
    rec_inv = lax.rsqrt(total[:, 0:1] / (rec_ref.shape[1] * n) + EPS)
    att_inv = lax.rsqrt(total[:, 4:5] / (att_ref.shape[1] * n) + EPS)
    rec_norm[...] = (rec_ref[...] * rec_inv * rgain_ref[...]).astype(jnp.bfloat16)
    att_norm[...] = (att_ref[...] * att_inv * again_ref[...]).astype(jnp.bfloat16)
    partner = group * 2 + (1 - core)
    first, second = [], []

    def cross(k):
        first[k].wait()
        pair = part[k, core].astype(jnp.float32) + rx1[k].astype(jnp.float32)
        tx2[k] = pair.astype(jnp.bfloat16)
        for e in range(1, groups):
            other = lax.rem(group + e, groups)
            second.append(
                pltpu.make_async_remote_copy(
                    src_ref=tx2.at[k, other], dst_ref=rx2.at[k, e - 1],
                    send_sem=s2.at[k, e - 1], recv_sem=r2.at[k, e - 1],
                    device_id={"tp": other * 2 + core}, device_id_type=MESH,
                )
            )
            second[-1].start()

    step = min(cols, 256)
    for k in range(chunks):
        for at in range(0, cols, step):
            here = slice(k * cols + at, k * cols + at + step)
            piece = (
                jnp.dot(rec_norm[...], wrec_ref[:, here], preferred_element_type=jnp.float32)
                + jnp.dot(att_norm[...], watt_ref[:, here], preferred_element_type=jnp.float32)
            ).astype(jnp.bfloat16)
            for j in range(n):
                part[k, j % 2, j // 2, :, at : at + step] = piece[j * block : (j + 1) * block]
        first.append(
            pltpu.make_async_remote_copy(
                src_ref=part.at[k, 1 - core], dst_ref=rx1.at[k], send_sem=s1.at[k],
                recv_sem=r1.at[k], device_id={"tp": partner}, device_id_type=MESH,
            )
        )
        first[-1].start()
        if k > 0:
            cross(k - 1)
    cross(chunks - 1)
    squares = jnp.zeros((block, 1), jnp.float32)
    for k in range(chunks):
        value = tx2[k, group].astype(jnp.float32)
        for e in range(1, groups):
            second[k * (groups - 1) + e - 1].wait()
            value = value + rx2[k, e - 1].astype(jnp.float32)
        mixed[k] = value
        squares = squares + jnp.sum(value * value, axis=1, keepdims=True)
    inverse = lax.rsqrt(squares / (chunks * cols) + EPS)
    for k in range(chunks):
        here = slice(k * cols, (k + 1) * cols)
        out_ref[:, here] = (mixed[k] * inverse * post_ref[:, here]).astype(jnp.bfloat16)


def project_out(rec_out, att_out, rec_gain, att_gain, w_out_rec, w_out_att, post_gain):
    n = lax.axis_size("tp")
    rows, channels = rec_out.shape
    width = w_out_rec.shape[1]
    chunks = math.gcd(width // 128, 4)
    cols, block, groups = width // chunks, rows // n, n // 2
    vmem = pl.BlockSpec(memory_space=pltpu.VMEM)
    low, dma = jnp.bfloat16, pltpu.SemaphoreType.DMA
    far = max(groups - 1, 1)
    return pl.pallas_call(
        functools.partial(out_kernel, n),
        out_shape=jax.ShapeDtypeStruct((block, width), low),
        in_specs=[vmem] * 7,
        out_specs=vmem,
        scratch_shapes=[
            pltpu.VMEM((rows, channels), low),
            pltpu.VMEM(att_out.shape, low),
            pltpu.VMEM((8, rows), jnp.float32),
            pltpu.VMEM((n - 1, 8, rows), jnp.float32),
            pltpu.VMEM((chunks, 2, groups, block, cols), low),
            pltpu.VMEM((chunks, groups, block, cols), low),
            pltpu.VMEM((chunks, groups, block, cols), low),
            pltpu.VMEM((chunks, far, block, cols), low),
            pltpu.VMEM((chunks, block, cols), jnp.float32),
            dma((n - 1,)),
            dma((n - 1,)),
            dma((chunks,)),
            dma((chunks,)),
            dma((chunks, far)),
            dma((chunks, far)),
        ],
        compiler_params=pltpu.CompilerParams(collective_id=1, has_side_effects=True),
        cost_estimate=pl.CostEstimate(
            flops=4 * rows * channels * width, bytes_accessed=8_000_000, transcendentals=0
        ),
        name="project_out",
    )(rec_out, att_out, rec_gain[None, :], att_gain[None, :], w_out_rec, w_out_att, post_gain[None, :])


def attend_kernel(
    n, m, q_ref, lat_ref, wexp_ref, out_ref,
    buf, peak, total, accum, p_s, p_r, y_s, y_r, c_s, c_r,
):
    me, tp = lax.axis_index("sp"), lax.axis_index("tp")
    core, group, groups = lax.rem(tp, 2), tp // 2, m // 2
    partner = group * 2 + (1 - core)
    pieces, block, wide = lat_ref.shape
    rows = pieces * block
    latent = wexp_ref.shape[0]
    heads = wexp_ref.shape[1] // (NOPE + VDIM)
    scaling = 1.0 / math.sqrt(NOPE + ROPE)
    barrier = pltpu.get_barrier_semaphore()
    for d in range(1, n):
        pl.semaphore_signal(
            barrier, inc=1, device_id={"sp": lax.rem(me + d, n)}, device_id_type=MESH
        )
    for e in range(1, groups):
        pl.semaphore_signal(
            barrier, inc=1, device_id={"tp": lax.rem(group + e, groups) * 2 + core},
            device_id_type=MESH,
        )
    pl.semaphore_signal(barrier, inc=1, device_id={"tp": partner}, device_id_type=MESH)
    pl.semaphore_wait(barrier, n - 1 + groups)

    def ahead(d):
        return pltpu.make_async_remote_copy(
            src_ref=lat_ref.at[tp], dst_ref=buf.at[d, tp], send_sem=p_s.at[d], recv_sem=p_r.at[d],
            device_id={"sp": lax.rem(me + d, n)}, device_id_type=MESH,
        )

    def across(d, e):
        return pltpu.make_async_remote_copy(
            src_ref=buf.at[d, tp], dst_ref=buf.at[d, tp], send_sem=y_s.at[d, e],
            recv_sem=y_r.at[d, e], device_id={"tp": lax.rem(group + e, groups) * 2 + core},
            device_id_type=MESH,
        )

    def inside(d, e):
        piece = lax.rem(group - e + groups, groups) * 2 + core
        return pltpu.make_async_remote_copy(
            src_ref=buf.at[d, piece], dst_ref=buf.at[d, piece], send_sem=c_s.at[d, e],
            recv_sem=c_r.at[d, e], device_id={"tp": partner}, device_id_type=MESH,
        )

    def send_one(d, carry):
        @pl.when(me + d < n)
        def _():
            ahead(d).start()

        return carry

    lax.fori_loop(1, n, send_one, 0)

    def chunk(lat, own):
        expanded = jnp.dot(
            lat[:, :latent], wexp_ref[...], preferred_element_type=jnp.float32
        ).astype(jnp.bfloat16)
        key_rope = lat[:, latent:]
        for h in range(heads):
            base = h * (NOPE + VDIM)
            keys = jnp.concatenate([expanded[:, base : base + NOPE], key_rope], axis=1)
            width = keys.shape[1]
            scores = lax.dot_general(
                q_ref[:, h * width : (h + 1) * width], keys, (((1,), (1,)), ((), ())),
                preferred_element_type=jnp.float32,
            ) * scaling
            if own:
                at_row = lax.broadcasted_iota(jnp.int32, scores.shape, 0)
                at_col = lax.broadcasted_iota(jnp.int32, scores.shape, 1)
                scores = jnp.where(at_col <= at_row, scores, -jnp.inf)
            high = jnp.max(scores, axis=1, keepdims=True)
            if not own:
                high = jnp.maximum(high, peak[h])
            weights = jnp.exp(scores - high)
            added = jnp.sum(weights, axis=1, keepdims=True)
            mixed = jnp.dot(
                weights.astype(jnp.bfloat16), expanded[:, base + NOPE : base + NOPE + VDIM],
                preferred_element_type=jnp.float32,
            )
            if not own:
                shrink = jnp.exp(peak[h] - high)
                added = added + total[h] * shrink
                mixed = mixed + accum[h] * shrink
            peak[h] = high
            total[h] = added
            accum[h] = mixed

    chunk(lat_ref[...].reshape(rows, wide), True)

    def step(t, carry):
        @pl.when(t <= me)
        def _():
            ahead(t).wait_recv()
            for e in range(1, groups):
                across(t, e).start()
            inside(t, 0).start()

        @pl.when((t >= 2) & (t - 1 <= me))
        def _():
            for e in range(1, groups):
                across(t - 1, e).wait_recv()
                inside(t - 1, e).start()

        @pl.when((t >= 3) & (t - 2 <= me))
        def _():
            for e in range(groups):
                inside(t - 2, e).wait_recv()
            chunk(buf[t - 2].reshape(rows, wide), False)

        return carry

    lax.fori_loop(1, n + 2, step, 0)
    for h in range(heads):
        out_ref[:, h * VDIM : (h + 1) * VDIM] = accum[h] / total[h]

    def finish(d, carry):
        @pl.when(me + d < n)
        def _():
            ahead(d).wait_send()

        @pl.when(d <= me)
        def _():
            for e in range(1, groups):
                across(d, e).wait_send()
            for e in range(groups):
                inside(d, e).wait_send()

        return carry

    lax.fori_loop(1, n, finish, 0)


def attend(query, latent_rope, w_expand):
    n, m = lax.axis_size("sp"), lax.axis_size("tp")
    rows, wide = latent_rope.shape
    heads = w_expand.shape[1] // (NOPE + VDIM)
    vmem = pl.BlockSpec(memory_space=pltpu.VMEM)
    dma = pltpu.SemaphoreType.DMA
    block = rows // m
    return pl.pallas_call(
        functools.partial(attend_kernel, n, m),
        out_shape=jax.ShapeDtypeStruct((rows, heads * VDIM), jnp.float32),
        in_specs=[vmem] * 3,
        out_specs=vmem,
        scratch_shapes=[
            pltpu.VMEM((n, m, block, wide), jnp.bfloat16),
            pltpu.VMEM((heads, rows, 1), jnp.float32),
            pltpu.VMEM((heads, rows, 1), jnp.float32),
            pltpu.VMEM((heads, rows, VDIM), jnp.float32),
            dma((n,)),
            dma((n,)),
            dma((n, m // 2)),
            dma((n, m // 2)),
            dma((n, m // 2)),
            dma((n, m // 2)),
        ],
        compiler_params=pltpu.CompilerParams(collective_id=2, has_side_effects=True),
        cost_estimate=pl.CostEstimate(
            flops=2_000_000_000, bytes_accessed=4_000_000, transcendentals=0
        ),
        name="attend",
    )(query, latent_rope.reshape(m, block, wide), w_expand)


def project_kernel(
    n, tok_ref, gain_ref, lgain_ref, wrope_ref, w_in, w_gate, w_query, w_latent,
    rec_ref, gate_ref, query_ref, latent_ref, rope_ref,
    buf, v_in, v_gate, v_query, v_latent, a_in, a_latent, w_sem, y_s, y_r, c_s, c_r,
):
    tp = lax.axis_index("tp")
    core, group, groups = lax.rem(tp, 2), tp // 2, n // 2
    partner = group * 2 + (1 - core)
    parts, sub, depth = tok_ref.shape
    rows = parts * sub
    loads = []
    for i, (src, dst) in enumerate(
        ((w_in, v_in), (w_gate, v_gate), (w_query, v_query), (w_latent, v_latent))
    ):
        loads.append(pltpu.make_async_copy(src, dst, w_sem.at[i]))
        loads[-1].start()
    barrier = pltpu.get_barrier_semaphore()
    for e in range(1, groups):
        pl.semaphore_signal(
            barrier, inc=1, device_id={"tp": lax.rem(group + e, groups) * 2 + core},
            device_id_type=MESH,
        )
    pl.semaphore_signal(barrier, inc=1, device_id={"tp": partner}, device_id_type=MESH)
    pl.semaphore_wait(barrier, groups)

    def origin(e):
        return lax.rem(group - e + groups, groups) * 2

    def across(e, r):
        return pltpu.make_async_remote_copy(
            src_ref=tok_ref.at[r], dst_ref=buf.at[tp, r], send_sem=y_s.at[e, r],
            recv_sem=y_r.at[e, r], device_id={"tp": lax.rem(group + e, groups) * 2 + core},
            device_id_type=MESH,
        )

    def inside(e, r):
        piece = origin(e) + core
        return pltpu.make_async_remote_copy(
            src_ref=tok_ref.at[r] if e == 0 else buf.at[piece, r], dst_ref=buf.at[piece, r],
            send_sem=c_s.at[e, r], recv_sem=c_r.at[e, r], device_id={"tp": partner},
            device_id_type=MESH,
        )

    for e in range(1, groups):
        for r in range(parts):
            across(e, r).start()
    for r in range(parts):
        inside(0, r).start()

    def multiply(values, piece, first):
        wide = values.reshape(rows, depth).astype(jnp.float32)
        scaled = (wide * gain_ref[piece]).astype(jnp.bfloat16)
        here = pl.ds(pl.multiple_of(piece * depth, depth), depth)
        for weight, total in (
            (v_in, a_in), (v_gate, gate_ref), (v_query, query_ref),
            (v_latent, a_latent), (wrope_ref, rope_ref),
        ):
            product = jnp.dot(scaled, weight[here, :], preferred_element_type=jnp.float32)
            total[...] = product if first else total[...] + product
        return jnp.sum(wide * wide, axis=1, keepdims=True)

    for load in loads:
        load.wait()
    squares = multiply(tok_ref[...], tp, True)
    for r in range(parts):
        inside(0, r).wait_recv()
    squares = squares + multiply(buf[partner], partner, False)
    for e in range(1, groups):
        for r in range(parts):
            across(e, r).wait_recv()
            inside(e, r).start()
        squares = squares + multiply(buf[origin(e) + core], origin(e) + core, False)
        for r in range(parts):
            inside(e, r).wait_recv()
        squares = squares + multiply(buf[origin(e) + 1 - core], origin(e) + 1 - core, False)
    inverse = lax.rsqrt(squares / (depth * n) + EPS)
    rec_ref[...] = (inverse * a_in[...]).astype(jnp.bfloat16)
    gate_ref[...] = inverse * gate_ref[...]
    query_ref[...] = inverse * query_ref[...]
    rope_ref[...] = inverse * rope_ref[...]
    latent = inverse * a_latent[...]
    mean = jnp.mean(latent * latent, axis=1, keepdims=True)
    latent_ref[...] = (latent * lax.rsqrt(mean + EPS) * lgain_ref[...]).astype(jnp.bfloat16)
    for r in range(parts):
        inside(0, r).wait_send()
        for e in range(1, groups):
            across(e, r).wait_send()
            inside(e, r).wait_send()


def project_in(tokens, pre_gain, latent_gain, w_rope, w_in, w_gate, w_query, w_latent):
    n = lax.axis_size("tp")
    rows, depth = tokens.shape
    parts = math.gcd(rows // 16, 4)
    sub = rows // parts
    low, wide, dma = jnp.bfloat16, jnp.float32, pltpu.SemaphoreType.DMA
    vmem, anywhere = pl.BlockSpec(memory_space=pltpu.VMEM), pl.BlockSpec(memory_space=pl.ANY)

    def shape(weight, kind):
        return jax.ShapeDtypeStruct((rows, weight.shape[1]), kind)

    return pl.pallas_call(
        functools.partial(project_kernel, n),
        out_shape=(
            shape(w_in, low), shape(w_gate, wide), shape(w_query, wide),
            shape(w_latent, low), shape(w_rope, wide),
        ),
        in_specs=[vmem] * 4 + [anywhere] * 4,
        out_specs=(vmem,) * 5,
        scratch_shapes=[
            pltpu.VMEM((n, parts, sub, depth), low),
            pltpu.VMEM(w_in.shape, low),
            pltpu.VMEM(w_gate.shape, low),
            pltpu.VMEM(w_query.shape, low),
            pltpu.VMEM(w_latent.shape, low),
            pltpu.VMEM((rows, w_in.shape[1]), wide),
            pltpu.VMEM((rows, w_latent.shape[1]), wide),
            dma((4,)),
            dma((n // 2, parts)),
            dma((n // 2, parts)),
            dma((n // 2, parts)),
            dma((n // 2, parts)),
        ],
        compiler_params=pltpu.CompilerParams(collective_id=3, has_side_effects=True),
        cost_estimate=pl.CostEstimate(
            flops=3_000_000_000, bytes_accessed=14_000_000, transcendentals=0
        ),
        name="project_in",
    )(
        tokens.reshape(parts, sub, depth), pre_gain.reshape(n, 1, depth), latent_gain[None, :],
        w_rope, w_in, w_gate, w_query, w_latent,
    )


def shards(
    tokens,
    pre_gain,
    rate_factor,
    w_rec_in,
    w_rec_gate,
    conv_taps,
    rate_maps,
    input_maps,
    decay_param,
    w_query,
    w_latent,
    w_rope_key,
    latent_gain,
    w_expand,
    rec_gain,
    att_gain,
    w_out_rec,
    w_out_att,
    post_gain,
):
    row_count = tokens.shape[0]
    heads_here = w_query.shape[1] // (NOPE + ROPE)
    first_place = lax.axis_index("sp") * row_count
    rec_input, gate_value, query_raw, own_latent, rope_raw = project_in(
        tokens, pre_gain, latent_gain, w_rope_key, w_rec_in, w_rec_gate, w_query, w_latent
    )
    rec_out = recurrent(
        rec_input,
        conv_taps,
        rate_maps,
        input_maps,
        jax.nn.softplus(-decay_param)[None, :],
        rate_factor[:, None],
        gate_value,
    )
    cosine, sine_part = angles(row_count, first_place, ROPE)
    query_heads = query_raw.reshape(row_count, heads_here, NOPE + ROPE)
    low = jnp.bfloat16
    query_rope = rotate(query_heads[:, :, NOPE:], cosine[:, None, :], sine_part[:, None, :])
    fill = NOPE - ROPE
    query = jnp.concatenate(
        [query_heads[:, :, :NOPE], query_rope, jnp.zeros((row_count, heads_here, fill))], axis=-1
    ).astype(low)
    rope_key = rotate(rope_raw, cosine, sine_part).astype(low)
    latent_rope = jnp.concatenate(
        [own_latent, rope_key, jnp.zeros((row_count, fill), low)], axis=-1
    )
    att_out = attend(query.reshape(row_count, heads_here * 2 * NOPE), latent_rope, w_expand)
    return project_out(rec_out, att_out, rec_gain, att_gain, w_out_rec, w_out_att, post_gain)


def solution(mesh):
    placed = (
        P("sp", "tp"),
        P(),
        P("sp"),
        P(None, "tp"),
        P(None, "tp"),
        P(None, "tp"),
        P("tp", None, None),
        P("tp", None, None),
        P("tp"),
        P(None, "tp"),
        P(),
        P(),
        P(),
        P(None, "tp"),
        P("tp"),
        P("tp"),
        P("tp", None),
        P("tp", None),
        P(),
    )
    return jax.shard_map(
        shards, mesh=mesh, in_specs=placed, out_specs=P(("sp", "tp"), None), check_vma=False
    )
```
